512 devices in a mesh: grp: 2 (over y), kv: 64 (over z, core), tp: 4 (over x).
Axes of the slice: x: 4, y: 2, z: 32, core: 2. Of those that a mesh axis runs over, the one named last changes fastest.
The devices are a block of a 4x8x32 slice.
Arguments:
- tokens: bfloat16 [65536, 2048], P(('grp', 'kv')), parts along dimension 0, may hold values from -72 to 72
- w_query: bfloat16 [2048, 1024], P(None, 'tp'), may hold values from -0.125 to 0.125
- w_key: bfloat16 [2048, 256], P(None, 'tp'), may hold values from -0.125 to 0.125
- w_value: bfloat16 [2048, 256], P(None, 'tp'), may hold values from -0.125 to 0.125
- w_out: bfloat16 [1024, 2048], P('tp'), may hold values from -0.1875 to 0.1875
- selection: int32 [4, 1024, 32], P('tp', ('grp', 'kv')), parts along dimension 1, may hold values from -1 to 511, as said below
Outputs:
- attended_out: bfloat16 [65536, 2048], P(('grp', 'kv', 'tp')), parts along dimension 0
The draws below stay inside these ranges and needn't reach their ends.
There are 2 independent parts, one for each index of `grp`. The reference program is written for one: setup_inputs(seed, part) draws one part's arguments, and reference() takes and returns one part's arrays. A program takes and returns all parts, laid end to end along the dimension named above; an argument that names none is the same for every part. Nothing has to cross between parts.
Inputs may be any that keep to these rules, and one draw needn't show every extreme that they name: `selection`: entry 0 is the query block's own index; the others are distinct indices of earlier blocks, then -1 for unused entries. For one key head, the query blocks of one device's range together choose at most 2 distinct blocks of any other device's range, and some device reaches 2 in every draw.
All inputs are finite; a program needn't handle non-finite values.
Results may differ from the reference program's by a relative error of at most 0.028.
The reference program's roundings to bfloat16 on the way (of `queries`, `keys`, `values`, `weights` and `attended`) count: a program that leaves them out, or rounds other values in their place, can miss the bound.
Values may be sent and summed in bfloat16 or wider, within the bound.
A program may use at most 128 MiB of HBM per device.

```python
import jax
import jax.numpy as jnp
from jax import lax

D = 2048
HEADS = 16
KV_HEADS = 4
HEAD_DIM = 64
BLOCK = 64
TOPK = 32
CAP = 2
QB_DEV = 8
TOKENS = 32768
NQB = 512
N_TP = 4


def draw_tokens(key, part):
    normal_draw = jax.random.normal(jax.random.fold_in(key, 11), (TOKENS, D), jnp.float32)
    normal_draw = jnp.clip(normal_draw, -6.0, 6.0)
    return normal_draw.astype(jnp.bfloat16)


def draw_selection(key, part):
    per_dev = QB_DEV
    total_blocks = NQB
    devices = total_blocks // per_dev
    pair_score = jax.random.randint(jax.random.fold_in(key, 21), (KV_HEADS, devices, devices, per_dev), 0, 1 << 20) * per_dev + jnp.arange(per_dev)
    rank_in = jnp.sum((pair_score[..., None, :] > pair_score[..., :, None]).astype(jnp.int32), axis=-1)
    in_pair = rank_in < CAP
    popular = jax.random.randint(jax.random.fold_in(key, 22), (KV_HEADS, total_blocks), 0, 4) * 300
    noise_int = jax.random.randint(jax.random.fold_in(key, 23), (KV_HEADS, total_blocks, total_blocks), 0, 1000)
    block_ids = jnp.arange(total_blocks)
    owner_ids = block_ids // per_dev
    within_ids = block_ids % per_dev
    dev_of = block_ids // per_dev
    slot_of = block_ids % per_dev
    pair_here = in_pair[:, dev_of[:, None], owner_ids[None, :], within_ids[None, :]]
    remote = (owner_ids[None, :] < dev_of[:, None])[None] & pair_here
    earlier = (owner_ids[None, :] == dev_of[:, None]) & (within_ids[None, :] < slot_of[:, None])
    candidate = remote | earlier[None]
    forced = (owner_ids[None, :] == dev_of[:, None] - 1) & (slot_of == 1)[:, None] | (owner_ids[None, :] == dev_of[:, None] - devices // 2) & (slot_of == 2)[:, None]
    value_int = noise_int + popular[:, None, :] + 4096 * forced[None].astype(jnp.int32)
    score_int = jnp.where(candidate, value_int * total_blocks + block_ids, -1 - block_ids)
    top_scores, top_index = lax.top_k(score_int, TOPK - 1)
    others = jnp.where(top_scores >= 0, top_index, -1)
    own_block = jnp.broadcast_to(block_ids[None, :, None], (KV_HEADS, total_blocks, 1))
    return jnp.concatenate([own_block, others], axis=-1).astype(jnp.int32)


def level_of(key, extent, split, low, high):
    def one(axis_at, blocks):
        heights = jax.random.uniform(jax.random.fold_in(jax.random.fold_in(key, 6), axis_at), (blocks,), jnp.float32, low / len(split), high / len(split))
        return jnp.repeat(jnp.exp(heights), extent[axis_at] // blocks).reshape((-1,) + (1,) * (len(extent) - axis_at - 1))

    factor_of = one(*split[0])
    for cut in split[1:]:
        factor_of = factor_of * one(*cut)
    return factor_of


def noise(own_key, extent, deviation, bound, shards=(), kind=jnp.bfloat16):
    level = level_of(own_key, extent, shards, -0.22, 0.18) if shards else 1.0
    array = jax.random.normal(own_key, extent, jnp.float32) * deviation * level
    return jnp.minimum(jnp.maximum(array, -bound), bound).astype(kind)


def setup_inputs(seed: int = 0, part: int = 0) -> dict:
    splits = jax.random.split(jax.random.key(seed), 7)
    part_splits = jax.random.split(jax.random.fold_in(splits[6], part), 7)
    tokens = draw_tokens(jax.random.fold_in(jax.random.fold_in(splits[6], part), 71), part)
    w_query = noise(splits[1], (D, HEADS * HEAD_DIM), D ** -0.5, 0.125, ((1, 4),))
    w_key = noise(splits[2], (D, KV_HEADS * HEAD_DIM), D ** -0.5, 0.125, ((1, 4),))
    w_value = noise(splits[3], (D, KV_HEADS * HEAD_DIM), D ** -0.5, 0.125, ((1, 4),))
    w_out = noise(splits[4], (HEADS * HEAD_DIM, D), (HEADS * HEAD_DIM) ** -0.5, 0.1875, ((0, 4),))
    selection = draw_selection(jax.random.fold_in(jax.random.fold_in(splits[6], part), 71), part)
    return {"tokens": tokens, "w_query": w_query, "w_key": w_key, "w_value": w_value, "w_out": w_out, "selection": selection}


ROPE_BASE = 500000.0


def rotate(head_rows, positions):
    half = head_rows.shape[-1] // 2
    freqs = ROPE_BASE ** (-jnp.arange(half, dtype=jnp.float32) / half)
    angles = positions[:, None, None] * freqs
    cosine = jnp.cos(angles)
    sine = jnp.sin(angles)
    first = head_rows[..., :half]
    second = head_rows[..., half:]
    return jnp.concatenate([first * cosine - second * sine, second * cosine + first * sine], axis=-1)


def reference(tokens, w_query, w_key, w_value, w_out, selection):
    length = tokens.shape[0]
    positions = jnp.arange(length).astype(jnp.float32)
    queries = rotate(jnp.dot(tokens, w_query, preferred_element_type=jnp.float32).reshape(length, HEADS, HEAD_DIM), positions).astype(jnp.bfloat16)
    keys = rotate(jnp.dot(tokens, w_key, preferred_element_type=jnp.float32).reshape(length, KV_HEADS, HEAD_DIM), positions).astype(jnp.bfloat16)
    values = jnp.dot(tokens, w_value, preferred_element_type=jnp.float32).astype(jnp.bfloat16)
    key_blocks = jnp.transpose(keys.reshape(NQB, BLOCK, KV_HEADS, HEAD_DIM), (2, 0, 1, 3))
    value_blocks = jnp.transpose(values.reshape(NQB, BLOCK, KV_HEADS, HEAD_DIM), (2, 0, 1, 3))
    group = HEADS // KV_HEADS
    head_ids = jnp.arange(KV_HEADS)[:, None]
    offsets = jnp.arange(BLOCK).astype(jnp.int32)
    score_scale = HEAD_DIM ** -0.5

    def one_block(block_id):
        query_rows = lax.dynamic_slice_in_dim(queries, block_id * BLOCK, BLOCK, 0).reshape(BLOCK, KV_HEADS, group, HEAD_DIM)
        chosen_ids = lax.dynamic_index_in_dim(selection, block_id, 1, keepdims=False)
        safe_ids = jnp.maximum(chosen_ids, 0)
        picked_keys = key_blocks[head_ids, safe_ids].reshape(KV_HEADS, TOPK * BLOCK, HEAD_DIM)
        picked_values = value_blocks[head_ids, safe_ids].reshape(KV_HEADS, TOPK * BLOCK, HEAD_DIM)
        scores = jnp.einsum('qhgd,hkd->hgqk', query_rows.astype(jnp.float32), picked_keys.astype(jnp.float32)) * score_scale
        key_pos = (chosen_ids[:, :, None] * BLOCK + offsets).reshape(KV_HEADS, TOPK * BLOCK)
        live_keys = jnp.repeat(chosen_ids >= 0, BLOCK, axis=1)
        query_pos = block_id * BLOCK + offsets
        allowed = live_keys[:, None, None, :] & (key_pos[:, None, None, :] <= query_pos[None, None, :, None])
        scores = jnp.where(allowed, scores, -jnp.inf)
        top_score = jnp.max(scores, axis=-1, keepdims=True)
        expo = jnp.exp(scores - top_score)
        weights = (expo / jnp.sum(expo, axis=-1, keepdims=True)).astype(jnp.bfloat16)
        attended = jnp.einsum('hgqk,hkd->qhgd', weights.astype(jnp.float32), picked_values.astype(jnp.float32)).astype(jnp.bfloat16)
        return attended.reshape(BLOCK, HEADS * HEAD_DIM)

    attended = lax.map(one_block, jnp.arange(NQB).astype(jnp.int32)).reshape(length, HEADS * HEAD_DIM)
    width = HEADS * HEAD_DIM // N_TP
    summed = jnp.zeros((length, D), jnp.float32)
    for group_id in range(N_TP):
        partial_out = jnp.dot(attended[:, group_id * width:(group_id + 1) * width], w_out[group_id * width:(group_id + 1) * width], preferred_element_type=jnp.float32).astype(jnp.bfloat16)
        summed = summed + lax.optimization_barrier(partial_out).astype(jnp.float32)
    return summed.astype(jnp.bfloat16)
```

```python
import functools
import math

import jax
import jax.numpy as jnp
import numpy as np
from jax import lax
from jax.experimental import pallas as pl
from jax.experimental.pallas import tpu as pltpu
from jax.sharding import PartitionSpec as P

HEAD_DIM = 64
BLOCK = 64
ROPE_BASE = 500000.0
CORES = 2
LANES = 128
CHUNKS = 8
TILES = 8
TCOLS = 256
SCALE = math.log2(math.e) * HEAD_DIM**-0.5
NEG = float("-inf")


def kernel(
    nkv, ntp,
    tok, wq, wk, wv, wo, cr, sr, sel, cb, sb,
    out,
    tok_v, wq_v, wkv_v, wall, cr_v, sr_v, kv, qt, acc, mx, kvs, wt, sbuf, biasr, ownb, tab_v, tab_s,
    att, att_in, oacc, ov,
    in_sem, tok_sem, ring_send, ring_recv, sib_send, sib_recv, w_send, w_recv, w_sib, a_send, a_recv, o_sem, t_sem,
):
    rows = tok.shape[0]
    crows = rows // CHUNKS
    pairs = rows // LANES
    nchip = nkv // CORES
    far = nchip // 2
    me = lax.axis_index("kv")
    core = lax.rem(me, CORES)
    z = me // CORES
    g = lax.axis_index("tp")
    sibling = z * CORES + (1 - core)
    right, left, opposite = lax.rem(g + 1, ntp), lax.rem(g + ntp - 1, ntp), lax.rem(g + 2, ntp)

    def dev(dist, c):
        return lax.rem(z + dist + 2 * nchip, nchip) * CORES + c

    loads = [
        pltpu.make_async_copy(wk, wkv_v.at[pl.ds(0, HEAD_DIM)], in_sem.at[0]),
        pltpu.make_async_copy(wv, wkv_v.at[pl.ds(HEAD_DIM, HEAD_DIM)], in_sem.at[1]),
    ]
    tok_loads = [
        pltpu.make_async_copy(tok.at[pl.ds(i * LANES, LANES)], tok_v.at[pl.ds(i * LANES, LANES)], tok_sem.at[i])
        for i in range(pairs)
    ]
    cr_load = pltpu.make_async_copy(cr, cr_v, in_sem.at[2])
    sr_load = pltpu.make_async_copy(sr, sr_v, in_sem.at[3])
    wq_load = pltpu.make_async_copy(wq, wq_v, in_sem.at[4])
    wo_load = pltpu.make_async_copy(wo, wall.at[g], in_sem.at[5])
    loads[0].start()
    loads[1].start()
    tok_loads[0].start()
    cr_load.start()
    sr_load.start()
    for i in range(1, pairs):
        tok_loads[i].start()
    wq_load.start()
    wo_load.start()

    barrier = pltpu.get_barrier_semaphore()
    for target in ({"kv": dev(1, core)}, {"kv": dev(-1, core)}, {"kv": sibling}, {"tp": right}, {"tp": left}, {"tp": opposite}):
        pl.semaphore_signal(barrier, inc=1, device_id=target)

    def ring(way, t, ch, source):
        span = pl.ds(pl.multiple_of(source * rows + ch * crows, crows), crows)
        return pltpu.make_async_remote_copy(
            src_ref=kv.at[span], dst_ref=kv.at[span], send_sem=ring_send.at[way], recv_sem=ring_recv.at[way, t, ch],
            device_id={"kv": dev(1 if way == 0 else -1, core)},
        )

    def ring_source(way, t):
        return dev(-t if way == 0 else t, core)

    def to_sibling(t, ch, source):
        span = pl.ds(pl.multiple_of(source * rows + ch * crows, crows), crows)
        return pltpu.make_async_remote_copy(
            src_ref=kv.at[span], dst_ref=kv.at[span], send_sem=sib_send.at[0], recv_sem=sib_recv.at[t],
            device_id={"kv": sibling},
        )

    def wait_sibling(t, count):
        span = pl.ds(0, count)
        pltpu.make_async_remote_copy(
            src_ref=kv.at[span], dst_ref=kv.at[span], send_sem=sib_send.at[0], recv_sem=sib_recv.at[t],
            device_id={"kv": sibling},
        ).wait_recv()

    wrows = wall.shape[1]
    half = wrows // CORES
    quarter = half // 2

    def w_copy(group, first, count, sem, recv, target):
        span = pl.ds(pl.multiple_of(first, quarter), count)
        return pltpu.make_async_remote_copy(
            src_ref=wall.at[group, span], dst_ref=wall.at[group, span], send_sem=w_send.at[sem], recv_sem=recv,
            device_id=target,
        )

    h0 = core * half
    w1 = [
        w_copy(g, h0, half, 0, w_recv.at[0], {"tp": right}),
        w_copy(g, h0, half, 1, w_recv.at[1], {"tp": left}),
    ]
    w2 = [
        w_copy(left, h0, quarter, 2, w_recv.at[2], {"tp": right}),
        w_copy(right, h0 + quarter, quarter, 3, w_recv.at[3], {"tp": left}),
        w_copy(left, h0, half, 4, w_sib.at[0], {"kv": sibling}),
        w_copy(right, h0, half, 5, w_sib.at[1], {"kv": sibling}),
    ]
    w3 = [w_copy(opposite, h0, half, 6, w_sib.at[2], {"kv": sibling})]

    lane = lax.broadcasted_iota(jnp.int32, (1, LANES), 1)
    sign = jnp.where(lax.rem(lane, HEAD_DIM) < HEAD_DIM // 2, -1.0, 1.0)
    first_half = lax.rem(lane, HEAD_DIM) < HEAD_DIM // 2
    is_key = lane < HEAD_DIM
    cb_row = cb[pl.ds(me, 1), :]
    sb_row = sb[pl.ds(me, 1), :]

    def angles(i):
        span = pl.ds(i * LANES, LANES)
        cr_t, sr_t = cr_v[span, :], sr_v[span, :]
        cosine = cb_row * cr_t - sb_row * sr_t
        sine = (sb_row * cr_t + cb_row * sr_t) * sign
        return cosine, sine

    def swapped(x):
        return jnp.where(first_half, pltpu.roll(x, LANES - HEAD_DIM // 2, 1), pltpu.roll(x, HEAD_DIM // 2, 1))

    loads[0].wait()
    loads[1].wait()
    for i in range(pairs):
        tok_loads[i].wait()
        x = lax.dot_general(
            tok_v[pl.ds(i * LANES, LANES), :], wkv_v[...], (((1,), (1,)), ((), ())), preferred_element_type=jnp.float32
        )
        if i == 0:
            cr_load.wait()
            sr_load.wait()
        cosine, sine = angles(i)
        rotated = x * jnp.where(is_key, cosine, 1.0) + swapped(x) * jnp.where(is_key, sine, 0.0)
        kv[pl.ds(pl.multiple_of(me * rows + i * LANES, LANES), LANES), :] = rotated.astype(jnp.bfloat16)
        if i == 0:
            pl.semaphore_wait(barrier, 6)
        for ch in range(i * LANES // crows, (i + 1) * LANES // crows):
            ring(0, 1, ch, me).start()
            ring(1, 1, ch, me).start()
            to_sibling(0, ch, me).start()
    wo_load.wait()
    for copy in w1:
        copy.start()

    nblocks = rows // BLOCK
    chosen = sel[0]
    lanes8 = lax.broadcasted_iota(jnp.int32, (nblocks, LANES), 1)
    bits = jnp.zeros((nblocks, LANES), jnp.int32)
    for t in range(chosen.shape[1]):
        entry = jnp.broadcast_to(chosen[:, t : t + 1], (nblocks, LANES))
        for j in range(nblocks):
            bits = bits | jnp.where(entry == lanes8 * nblocks + j, 1 << j, 0)
    union = bits[0:1]
    for b in range(1, nblocks):
        union = union | bits[b : b + 1]
    union = jnp.broadcast_to(union, (nblocks, LANES))
    low = union & (-union)
    rest = union & ~low
    low2 = rest & (-rest)
    index = jnp.zeros_like(union)
    for j in range(1, nblocks):
        index = index + jnp.where(low == (1 << j), j, 0) + jnp.where(low2 == (1 << j), j * 256, 0)
    tab_v[0:8, :] = bits
    tab_v[8:16, :] = index
    tab_copy = pltpu.make_async_copy(tab_v, tab_s, t_sem.at[0])
    tab_copy.start()
    for slot, bit in enumerate((low, low2)):
        open_ = jnp.where((bits & bit) != 0, 0.0, NEG)
        turned = open_.T[:nkv]
        for p in range(pairs):
            biasr[slot * pairs + p] = jnp.where(
                is_key,
                jnp.broadcast_to(turned[:, 2 * p : 2 * p + 1], (nkv, LANES)),
                jnp.broadcast_to(turned[:, 2 * p + 1 : 2 * p + 2], (nkv, LANES)),
            )

    wq_load.wait()
    heads = wq_v.shape[1] // HEAD_DIM
    for i in range(pairs):
        x = jnp.dot(tok_v[pl.ds(i * LANES, LANES), :], wq_v[...], preferred_element_type=jnp.float32)
        cosine, sine = angles(i)
        for hp in range(heads // 2):
            part = x[:, hp * LANES : (hp + 1) * LANES]
            rotated = (part * cosine + swapped(part) * sine).astype(jnp.bfloat16).astype(jnp.float32)
            flipped = rotated.T.astype(jnp.bfloat16)
            u = i * 2 + hp
            qt[u, 0:HEAD_DIM, 0:LANES] = flipped[:HEAD_DIM]
            qt[u, 0:HEAD_DIM, LANES:TCOLS] = flipped[HEAD_DIM:]
            qt[u, HEAD_DIM:LANES, :] = jnp.zeros((LANES - HEAD_DIM, TCOLS), jnp.bfloat16)

    tab_copy.wait()
    key_row = lax.broadcasted_iota(jnp.int32, (BLOCK, LANES), 0)
    query_col = lax.rem(lax.broadcasted_iota(jnp.int32, (BLOCK, LANES), 1), BLOCK)
    causal = jnp.where(key_row <= query_col, 0.0, NEG)
    for p in range(pairs):
        for j in range(2 * p + 2):
            sides = []
            for b in (2 * p, 2 * p + 1):
                if j > b:
                    sides.append(jnp.full((BLOCK, LANES), NEG, jnp.float32))
                else:
                    seen = (tab_s[b, me] >> j) & 1
                    gate = jnp.where(seen == 1, 0.0, NEG)
                    sides.append((causal if j == b else jnp.zeros((BLOCK, LANES), jnp.float32)) + gate)
            ownb[p, j * BLOCK : (j + 1) * BLOCK, :] = jnp.where(is_key, sides[0], sides[1])

    def chosen_blocks(source):
        packed = tab_s[8, source]
        i0, i1 = packed & 255, packed >> 8
        base = source * rows
        first = second = kv[pl.ds(pl.multiple_of(base, BLOCK), BLOCK), :]
        for j in range(1, nblocks):
            block = kv[pl.ds(pl.multiple_of(base + j * BLOCK, BLOCK), BLOCK), :]
            first = lax.select_n(i0 == j, first, block)
            second = lax.select_n(i1 == j, second, block)
        return first, second

    def gather(sources, at=0):
        for n, source in enumerate(sources):
            first, second = chosen_blocks(source)
            o = at + n * 2 * BLOCK
            kvs[o : o + BLOCK, :] = first
            kvs[o + BLOCK : o + 2 * BLOCK, :] = second

    def turn(count):
        values = jnp.where(lane < HEAD_DIM, jnp.ones((), jnp.bfloat16), kvs[0:count, :])
        wt[:, 0:count] = values.T

    def scores(u, count):
        sbuf[u % 2, 0:count, :] = jnp.dot(kvs[0:count, :], qt[u], preferred_element_type=jnp.float32)

    def twice(row):
        return jnp.concatenate([row, row], axis=1)

    def remote_bias(u, sources):
        found = []
        for source in sources:
            for slot in (0, 1):
                found.append(twice(biasr[slot * pairs + u // 2, pl.ds(source, 1), :]))
        return found

    def attend(u, count, biases, first=False):
        blocks, tops = [], []
        for k in range(count // BLOCK):
            sk = sbuf[u % 2, k * BLOCK : (k + 1) * BLOCK, :]
            bias = biases[k]
            if bias.shape[0] > 1:
                sk = sk + bias
                bias = None
            top = jnp.max(sk, axis=0, keepdims=True)
            tops.append(top if bias is None else top + bias)
            blocks.append((sk, bias))
        m_new = functools.reduce(jnp.maximum, tops)
        if not first:
            m_old = mx[u]
            m_new = jnp.maximum(m_new, m_old)
            alpha = jnp.exp2((m_old - m_new) * SCALE)
        probs = []
        for sk, bias in blocks:
            shift = m_new if bias is None else m_new - bias
            probs.append(jnp.exp2((sk - shift) * SCALE).astype(jnp.bfloat16))
        gained = jnp.dot(wt[:, 0:count], jnp.concatenate(probs, axis=0), preferred_element_type=jnp.float32)
        acc[u] = gained if first else acc[u] * alpha + gained
        mx[u] = m_new

    def receive(t, u, forward_up=True, forward_down=True):
        for way, forward in ((0, forward_up), (1, forward_down)):
            source = ring_source(way, t)
            ring(way, t, u, source).wait_recv()
            if forward is True:
                ring(way, t + 1, u, source).start()
            elif forward is not False:
                @pl.when(forward)
                def _():
                    ring(way, t + 1, u, source).start()
            to_sibling(t, u, source).start()

    for u in range(TILES):
        receive(1, u)
        p = u // 2
        own_keys = (2 * p + 2) * BLOCK
        count = own_keys + 2 * BLOCK
        if u == 0:
            wait_sibling(0, rows)
        if u % 2 == 0:
            kvs[0:own_keys, :] = kv[pl.ds(pl.multiple_of(me * rows, rows), own_keys), :]
            gather([sibling], own_keys)
            turn(count)
        scores(u, count)
        own = [
            jnp.concatenate([ownb[p, j * BLOCK : (j + 1) * BLOCK, :]] * 2, axis=1) for j in range(2 * p + 2)
        ]
        attend(u, count, own + remote_bias(u, [sibling]), first=True)

    def four(t):
        return [dev(-t, 0), dev(-t, 1), dev(t, 0), dev(t, 1)]

    def round_(t, receive_tile):
        sources = four(t - 1)
        count = len(sources) * 2 * BLOCK
        for u in range(TILES):
            receive_tile(u)
            if u == 0:
                wait_sibling(t - 1, 2 * rows)
                gather(sources)
                turn(count)
                scores(0, count)
            if u + 1 < TILES:
                scores(u + 1, count)
            attend(u, count, remote_bias(u, sources))

    def middle(t, carry):
        @pl.when(t == 6)
        def _():
            for copy in w1:
                copy.wait_recv()
            for copy in w2:
                copy.start()

        @pl.when(t == 11)
        def _():
            for copy in w2[:2]:
                copy.wait_recv()
            for copy in w3:
                copy.start()

        def receive_tile(u):
            more = t + 1 < far
            receive(t, u, True if u < CHUNKS // 2 else more, more if u < CHUNKS // 2 else True)

        round_(t, receive_tile)
        return carry

    lax.fori_loop(2, far, middle, 0)

    def last_receive(u):
        if u < CHUNKS // 2:
            for way, ch in ((0, u), (1, u + CHUNKS // 2)):
                source = ring_source(way, far)
                ring(way, far, ch, source).wait_recv()
                to_sibling(far, ch, source).start()

    round_(far, last_receive)

    sources = [dev(far, 0), dev(far, 1)]
    count = len(sources) * 2 * BLOCK
    wait_sibling(far, rows)
    gather(sources)
    turn(count)
    scores(0, count)

    def a_copy(pair, d):
        return pltpu.make_async_remote_copy(
            src_ref=att.at[pair], dst_ref=att_in.at[g], send_sem=a_send.at[d], recv_sem=a_recv.at[d],
            device_id={"tp": pair},
        )

    for u in range(TILES):
        if u + 1 < TILES:
            scores(u + 1, count)
        attend(u, count, remote_bias(u, sources))
        done = acc[u]
        share = (done[HEAD_DIM:] / done[:HEAD_DIM]).astype(jnp.bfloat16)
        pair, hp = u // 2, u % 2
        for hh in range(2):
            first = (hp * 2 + hh) * HEAD_DIM
            att[pair, first : first + HEAD_DIM, :] = share[:, hh * LANES : (hh + 1) * LANES]
        if hp == 1:
            @pl.when(pair != g)
            def _():
                a_copy(pair, lax.rem(pair - g + ntp, ntp)).start()

    for n in range(3):
        w_copy((left, right, opposite)[n], h0, half, 4 + n, w_sib.at[n], {"kv": sibling}).wait_recv()
    ocols = 512
    steps = ov.shape[1] // ocols
    for n, d in enumerate((0, 1, 3, 2)):
        source = lax.rem(g - d + ntp, ntp)
        if d == 0:
            part = att[g]
        else:
            pltpu.make_async_remote_copy(
                src_ref=att.at[g], dst_ref=att_in.at[source], send_sem=a_send.at[d], recv_sem=a_recv.at[d],
                device_id={"tp": source},
            ).wait_recv()
            part = att_in[source]
        part = part.T
        for s in range(steps):
            cols = pl.ds(s * ocols, ocols)
            product = jnp.dot(part, wall[source, :, cols], preferred_element_type=jnp.float32)
            product = product.astype(jnp.bfloat16).astype(jnp.float32)
            if n == 0:
                oacc[:, cols] = product
            elif n < 3:
                oacc[:, cols] = oacc[:, cols] + product
            else:
                ov[:, cols] = (oacc[:, cols] + product).astype(jnp.bfloat16)
                pltpu.make_async_copy(ov.at[:, cols], out.at[:, cols], o_sem.at[s]).start()

    for d in (1, 2, 3):
        a_copy(lax.rem(g + d, ntp), d).wait_send()
    for copy in w1 + w2 + w3:
        copy.wait_send()
    sent = rows * (far - 1) + rows // 2
    for way in (0, 1):
        span = pl.ds(0, sent)
        pltpu.make_async_remote_copy(
            src_ref=kv.at[span], dst_ref=kv.at[span], send_sem=ring_send.at[way], recv_sem=ring_recv.at[way, 0, 0],
            device_id={"kv": sibling},
        ).wait_send()
    span = pl.ds(0, rows * nchip)
    pltpu.make_async_remote_copy(
        src_ref=kv.at[span], dst_ref=kv.at[span], send_sem=sib_send.at[0], recv_sem=sib_recv.at[0],
        device_id={"kv": sibling},
    ).wait_send()
    for s in range(steps):
        cols = pl.ds(s * ocols, ocols)
        pltpu.make_async_copy(ov.at[:, cols], out.at[:, cols], o_sem.at[s]).wait()


def rotary_tables(rows, nkv):
    half = HEAD_DIM // 2
    freqs = ROPE_BASE ** (-np.arange(half, dtype=np.float64) / half)
    freqs = np.tile(freqs, LANES // half)[None, :]
    within = np.arange(rows, dtype=np.float64)[:, None] * freqs
    base = (np.arange(nkv, dtype=np.float64) * rows)[:, None] * freqs
    return [f(a).astype(np.float32) for a in (within, base) for f in (np.cos, np.sin)]


def solution(mesh):
    nkv, ntp = mesh.shape["kv"], mesh.shape["tp"]
    far = nkv // CORES // 2

    def shards(tokens, w_query, w_key, w_value, w_out, selection):
        rows, width = tokens.shape
        pairs = rows // LANES
        crow, srow, cbase, sbase = rotary_tables(rows, nkv)
        anywhere = pl.BlockSpec(memory_space=pl.ANY)
        vmem = pl.BlockSpec(memory_space=pltpu.VMEM)
        wide = w_out.shape[1]
        bf16, f32, i32 = jnp.bfloat16, jnp.float32, jnp.int32
        dma = pltpu.SemaphoreType.DMA
        return pl.pallas_call(
            functools.partial(kernel, nkv, ntp),
            out_shape=jax.ShapeDtypeStruct((rows // ntp, wide), bf16),
            in_specs=[anywhere] * 7 + [vmem] * 3,
            out_specs=anywhere,
            scratch_shapes=[
                pltpu.VMEM(tokens.shape, bf16),
                pltpu.VMEM(w_query.shape, bf16),
                pltpu.VMEM((2 * HEAD_DIM, width), bf16),
                pltpu.VMEM((ntp, *w_out.shape), bf16),
                pltpu.VMEM((rows, LANES), f32),
                pltpu.VMEM((rows, LANES), f32),
                pltpu.VMEM((nkv * rows, 2 * HEAD_DIM), bf16),
                pltpu.VMEM((TILES, LANES, TCOLS), bf16),
                pltpu.VMEM((TILES, LANES, TCOLS), f32),
                pltpu.VMEM((TILES, 1, TCOLS), f32),
                pltpu.VMEM((rows + 2 * BLOCK, LANES), bf16),
                pltpu.VMEM((LANES, rows + 2 * BLOCK), bf16),
                pltpu.VMEM((2, rows + 2 * BLOCK, TCOLS), f32),
                pltpu.VMEM((2 * pairs, nkv, LANES), f32),
                pltpu.VMEM((pairs, rows, LANES), f32),
                pltpu.VMEM((16, LANES), i32),
                pltpu.SMEM((16, LANES), i32),
                pltpu.VMEM((pairs, w_query.shape[1], LANES), bf16),
                pltpu.VMEM((pairs, w_query.shape[1], LANES), bf16),
                pltpu.VMEM((rows // ntp, wide), f32),
                pltpu.VMEM((rows // ntp, wide), bf16),
                dma((6,)),
                dma((pairs,)),
                dma((2,)),
                dma((2, far + 1, CHUNKS)),
                dma((1,)),
                dma((far + 1,)),
                dma((7,)),
                dma((4,)),
                dma((3,)),
                dma((ntp,)),
                dma((ntp,)),
                dma((wide // 512,)),
                dma((1,)),
            ],
            compiler_params=pltpu.CompilerParams(
                collective_id=0, has_side_effects=True, vmem_limit_bytes=60 * 1024 * 1024
            ),
        )(tokens, w_query, w_key.T, w_value.T, w_out, crow, srow, selection, cbase, sbase)

    placed = (
        P(("grp", "kv"), None),
        P(None, "tp"),
        P(None, "tp"),
        P(None, "tp"),
        P("tp", None),
        P("tp", ("grp", "kv"), None),
    )
    return jax.shard_map(
        shards, mesh=mesh, in_specs=placed, out_specs=P(("grp", "kv", "tp"), None), check_vma=False
    )
```
